768 devices in a mesh: ep: 48 (over z, x), tp: 16 (over y, core).
Axes of the slice: x: 4, y: 8, z: 12, core: 2. Of those that a mesh axis runs over, the one named last changes fastest.
Arguments:
- tokens: bfloat16 [6144, 2048], P('ep'), may hold values from -6 to 6
- routes: int32 [6144, 2], P('ep'), may hold values from 0 to 47, all different within a row; in each aligned block of 128 rows (0 to 127, 128 to 255, ...) at most 6 rows name the same one
- route_gates: float32 [6144, 2], P('ep'), may hold values from 0.1 to 2
- cotangent: bfloat16 [6144, 2048], P('ep'), may hold values from -40 to 40
- w_gate: bfloat16 [48, 2048, 1536], P('ep', None, 'tp'), may hold values from -0.125 to 0.125
- w_up: bfloat16 [48, 2048, 1536], P('ep', None, 'tp'), may hold values from -0.125 to 0.125
- w_down: bfloat16 [48, 1536, 2048], P('ep', 'tp'), may hold values from -0.15625 to 0.15625
- s_gate: bfloat16 [2048, 1536], P(None, 'tp'), may hold values from -0.125 to 0.125
- s_up: bfloat16 [2048, 1536], P(None, 'tp'), may hold values from -0.125 to 0.125
- s_down: bfloat16 [1536, 2048], P('tp'), may hold values from -0.15625 to 0.15625
Outputs:
- token_grad: bfloat16 [6144, 2048], P('ep', 'tp')
- gate_grad: float32 [6144, 2], P('ep')
- grad_gate: float32 [48, 2048, 1536], P('ep', None, 'tp')
- grad_up: float32 [48, 2048, 1536], P('ep', None, 'tp')
- grad_down: float32 [48, 1536, 2048], P('ep', 'tp')
- grad_shared: float32 [1536, 2048], P(('tp', 'ep'))
- norm_in: float32 [48, 2, 2048], P('ep')
- norm_down: float32 [48, 1536], P('ep', 'tp')
- norm_shared: float32 [1536], P(('tp', 'ep'))
The draws below stay inside these ranges and needn't reach their ends.
Inputs may be any that keep to these rules, and one draw needn't show every extreme that they name: `routes`: within the rows of one index of ep no expert is named by more than 6 assignments, a bound that some block reaches.
All inputs are finite; a program needn't handle non-finite values.
Results may differ from the reference program's by a relative error of at most 0.0095.
Values may be sent and summed in bfloat16 or wider, within the bound.
No kernel may reach another device: no remote copies, remote signals or barrier semaphores. Data moves between devices by JAX's collectives and lax.ppermute only.
A program may use at most 64 MiB of HBM per device.

```python
import math
import jax
import jax.numpy as jnp
import numpy as np
from jax import lax

D = 2048
FF = 1536
SHARED = 1536
TOP_K = 2
TOK_DEV = 128
EXPERTS = 48
CAP = 6
ROWS = 288
TOKENS = 6144
N_EP = 48
N_TP = 16


def draw_cotangent(key, part):
    first = jax.random.fold_in(key, 11)
    second = jax.random.fold_in(key, 12)
    third = jax.random.fold_in(key, 13)
    values = jax.random.normal(first, (TOKENS, D), jnp.float32)
    column_scale = jnp.exp(jax.random.uniform(third, (1, D), jnp.float32, math.log(0.3), math.log(3.0)))
    row_scale = jnp.exp(jax.random.uniform(second, (TOKENS, 1), jnp.float32, math.log(0.3), math.log(3.0)))
    values = jnp.clip(values, -5.0, 5.0)
    return (0.3 * values * row_scale * column_scale).astype(jnp.bfloat16)


def shard_levels(own_key, dims, shards, least, largest):
    def one(dim, blocks):
        steps = jax.random.uniform(jax.random.fold_in(jax.random.fold_in(own_key, 6), dim), (blocks,), jnp.float32, least / len(shards), largest / len(shards))
        return jnp.repeat(jnp.exp(steps), dims[dim] // blocks).reshape((-1,) + (1,) * (len(dims) - dim - 1))

    gain = one(*shards[0])
    for cut in shards[1:]:
        gain = gain * one(*cut)
    return gain


def routed_block(rng, own, number, rows, amount, top, bound, slope):
    order = jax.random.permutation(rng, amount)
    crowded, ordinary = portions_of(amount, rows * top, bound, slope, True), portions_of(amount, rows * top, bound, slope, False)
    places = jnp.arange(amount)

    def named(sizes, turn):
        used = int((sizes > 0).sum())
        fixed = max(1, used // 4)
        shifted = fixed + (places - fixed + turn * (used - fixed)) % max(1, amount - fixed)
        return jnp.zeros((amount,), jnp.int32).at[order[jnp.where(places < fixed, places, shifted)]].set(jnp.asarray(sizes, jnp.int32))

    sizes = jnp.where(number % 4 == 0, named(crowded, number // 4), named(ordinary, number - number // 4 - 1))
    mixed = jax.random.permutation(jax.random.fold_in(own, 3), amount)
    donor, taker = mixed[0:amount // 2 * 2:2], mixed[1:amount // 2 * 2:2]
    slack = jnp.minimum(sizes[donor] - 1, bound - sizes[taker]) // 2
    slack = jnp.where((donor == order[0]) | (taker == order[0]) | (sizes[taker] == 0), 0, jnp.maximum(slack, 0))
    shifted = jax.random.randint(jax.random.fold_in(own, 4), (amount // 2,), 0, 1 << 20) % (slack + 1)
    sizes = sizes.at[donor].add(-shifted).at[taker].add(shifted)
    labels = jnp.searchsorted(jnp.cumsum(sizes), jnp.arange(rows * top), side="right").astype(jnp.int32)
    listing = labels.reshape(top, rows).T
    listing = listing[jax.random.permutation(jax.random.fold_in(own, 1), rows)]
    turn = jax.random.randint(jax.random.fold_in(own, 2), (rows, 1), 0, top)
    return jnp.take_along_axis(listing, (jnp.arange(top)[None, :] + turn) % top, axis=1)


def portions_of(number_of, total, reach, lean, full):
    portions = [(1 << 20) // math.isqrt(rank ** lean) + 1 for rank in range(1, number_of + 1)]
    largest = reach if full else min(reach, max(-(-total // number_of), total * portions[0] // sum(portions)))
    least = 1 if total - largest >= number_of - 1 else 0
    given, surplus = [largest] + [least] * (number_of - 1), total - largest - least * (number_of - 1)
    while surplus > 0:
        movable = [i for i in range(1, number_of) if given[i] < largest] or [i for i in range(1, number_of) if given[i] < reach]
        pool, budget = sum([portions[i] for i in movable]), surplus
        for i in movable:
            addition = min(reach - given[i], max(1, budget * portions[i] // pool), surplus)
            given[i] = given[i] + addition
            surplus = surplus - addition
    return np.array(given)


def centred(stream_key, shape, scale, bound, shards=(), kind=jnp.bfloat16):
    drawn = jax.random.normal(stream_key, shape, jnp.float32) * scale
    if len(shards) > 0:
        drawn = shard_levels(stream_key, shape, shards, -0.22, 0.18) * drawn
    return jnp.clip(drawn, min=-bound, max=bound).astype(kind)


def setup_inputs(seed: int = 0) -> dict:
    arg_keys = jax.random.split(jax.random.key(seed), 11)
    tokens = centred(arg_keys[0], (TOKENS, D), 1.0, 6.0, ((0, 48),))
    routes_keys = jax.random.split(jax.random.fold_in(arg_keys[1], 1), TOKENS // TOK_DEV)
    routes_turns = jax.random.permutation(jax.random.fold_in(arg_keys[1], 3), TOKENS // TOK_DEV)
    routes = jax.vmap(lambda own, number: routed_block(jax.random.fold_in(arg_keys[1], 2), own, number, TOK_DEV, EXPERTS, TOP_K, CAP, 1))(routes_keys, routes_turns).reshape((TOKENS, TOP_K))
    route_gates = jnp.clip(jnp.exp(math.log(2.0) - 2.9957323 * jax.random.uniform(arg_keys[2], (TOKENS, TOP_K), jnp.float32) ** shard_levels(arg_keys[2], (TOKENS, TOP_K), ((0, 48),), -0.2, 0.2)), 0.1, 2.0)
    cotangent = draw_cotangent(jax.random.fold_in(arg_keys[10], 71), 0)
    w_gate = centred(arg_keys[4], (EXPERTS, D, FF), D ** -0.5, 0.125, ((0, 48), (2, 16)))
    w_up = centred(arg_keys[5], (EXPERTS, D, FF), D ** -0.5, 0.125, ((0, 48), (2, 16)))
    w_down = centred(arg_keys[6], (EXPERTS, FF, D), FF ** -0.5, 0.15625, ((0, 48), (1, 16)))
    s_gate = centred(arg_keys[7], (D, SHARED), D ** -0.5, 0.125, ((1, 16),))
    s_up = centred(arg_keys[8], (D, SHARED), D ** -0.5, 0.125, ((1, 16),))
    s_down = centred(arg_keys[9], (SHARED, D), SHARED ** -0.5, 0.15625, ((0, 16),))
    return {"tokens": tokens, "routes": routes, "route_gates": route_gates, "cotangent": cotangent, "w_gate": w_gate, "w_up": w_up, "w_down": w_down, "s_gate": s_gate, "s_up": s_up, "s_down": s_down}


def slot_table(routes):
    chosen = routes.reshape(N_EP, TOK_DEV * TOP_K)
    expert_ids = jnp.arange(EXPERTS, dtype=jnp.int32)
    one_hot = (chosen[:, :, None] == expert_ids[None, None, :]).astype(jnp.int32)
    ranks = jnp.sum((jnp.cumsum(one_hot, axis=1) - one_hot) * one_hot, axis=2)
    source = jnp.arange(N_EP, dtype=jnp.int32)[:, None]
    slot_of = chosen * ROWS + source * CAP + ranks
    return slot_of.reshape(TOKENS * TOP_K).astype(jnp.int32)


def block_sum(d_gate, d_up, gate_weight, up_weight):
    block_width = gate_weight.shape[1] // N_TP
    running = jnp.zeros((d_gate.shape[0], gate_weight.shape[0]), jnp.float32)
    for block_index in range(N_TP):
        lower = block_index * block_width
        upper = lower + block_width
        block_term = jnp.dot(d_gate[:, lower:upper], gate_weight[:, lower:upper].T, preferred_element_type=jnp.float32)
        block_term = block_term + jnp.dot(d_up[:, lower:upper], up_weight[:, lower:upper].T, preferred_element_type=jnp.float32)
        rounded = lax.optimization_barrier(block_term.astype(jnp.bfloat16))
        running = running + rounded.astype(jnp.float32)
    return running


def swiglu_back(rows_x, rows_c, gate_weight, up_weight, down_weight):
    pre_gate = jnp.dot(rows_x, gate_weight, preferred_element_type=jnp.float32)
    pre_up = jnp.dot(rows_x, up_weight, preferred_element_type=jnp.float32)
    sigmoid_gate = jax.nn.sigmoid(pre_gate)
    activated = pre_gate * sigmoid_gate
    hidden = (activated * pre_up).astype(jnp.bfloat16)
    hidden_grad = jnp.dot(rows_c, down_weight.T, preferred_element_type=jnp.float32)
    d_gate = (hidden_grad * pre_up * sigmoid_gate * (1.0 + pre_gate * (1.0 - sigmoid_gate))).astype(jnp.bfloat16)
    d_up = (hidden_grad * activated).astype(jnp.bfloat16)
    return hidden, hidden_grad, d_gate, d_up


def expert_back(args):
    rows_x, rows_c, gate_weight, up_weight, down_weight = args
    hidden, hidden_grad, d_gate, d_up = swiglu_back(rows_x, rows_c, gate_weight, up_weight, down_weight)
    gate_dot = jnp.sum(hidden.astype(jnp.float32) * hidden_grad, axis=1).astype(jnp.bfloat16)
    grad_gate = jnp.dot(rows_x.T, d_gate, preferred_element_type=jnp.float32)
    grad_up = jnp.dot(rows_x.T, d_up, preferred_element_type=jnp.float32)
    grad_down = jnp.dot(hidden.T, rows_c, preferred_element_type=jnp.float32)
    slot_grad = block_sum(d_gate, d_up, gate_weight, up_weight)
    return grad_gate, grad_up, grad_down, slot_grad, gate_dot


def reference(tokens, routes, route_gates, cotangent, w_gate, w_up, w_down, s_gate, s_up, s_down):
    slot_of = slot_table(routes)
    token_of = (jnp.arange(TOKENS * TOP_K, dtype=jnp.int32) // TOP_K).astype(jnp.int32)
    row_token = jnp.full((EXPERTS * ROWS,), TOKENS, jnp.int32).at[slot_of].set(token_of)
    row_gate = jnp.zeros((EXPERTS * ROWS,), jnp.float32).at[slot_of].set(route_gates.reshape(TOKENS * TOP_K))
    padded_x = jnp.concatenate([tokens, jnp.zeros((1, D), jnp.bfloat16)], axis=0)
    padded_c = jnp.concatenate([cotangent, jnp.zeros((1, D), jnp.bfloat16)], axis=0)
    slot_x = padded_x[row_token].reshape(EXPERTS, ROWS, D)
    slot_c = (row_gate[:, None] * padded_c[row_token].astype(jnp.float32)).astype(jnp.bfloat16).reshape(EXPERTS, ROWS, D)
    grad_gate, grad_up, grad_down, slot_grad, gate_dot = lax.map(expert_back, (slot_x, slot_c, w_gate, w_up, w_down))
    routed = jax.ops.segment_sum(slot_grad.reshape(EXPERTS * ROWS, D), row_token, num_segments=TOKENS + 1)[:TOKENS]
    gate_grad = gate_dot.reshape(EXPERTS * ROWS)[slot_of].reshape(TOKENS, TOP_K).astype(jnp.float32) / route_gates
    s_hidden, s_hidden_grad, s_d_gate, s_d_up = swiglu_back(tokens, cotangent, s_gate, s_up, s_down)
    grad_shared = jnp.dot(s_hidden.T, cotangent, preferred_element_type=jnp.float32)
    shared_back = block_sum(s_d_gate, s_d_up, s_gate, s_up)
    token_grad = (shared_back + routed).astype(jnp.bfloat16)
    norm_in = jnp.stack([jnp.mean(grad_gate ** 2, axis=2), jnp.mean(grad_up ** 2, axis=2)], axis=1)
    norm_down = jnp.mean(grad_down ** 2, axis=2)
    norm_shared = jnp.mean(grad_shared ** 2, axis=1)
    return (token_grad, gate_grad, grad_gate, grad_up, grad_down, grad_shared, norm_in, norm_down, norm_shared)
```

```python
import functools

import jax
import jax.numpy as jnp
from jax import lax
from jax.experimental import pallas as pl
from jax.experimental.pallas import tpu as pltpu
from jax.sharding import Mesh, PartitionSpec as P

BF = jnp.bfloat16
F32 = jnp.float32
LANES = 128


def up(n, k):
    return -(-n // k) * k


def nn(a, b):
    return lax.dot_general(a, b, (((1,), (0,)), ((), ())), preferred_element_type=F32)


def nt(a, b):
    return lax.dot_general(a, b, (((1,), (1,)), ((), ())), preferred_element_type=F32)


def tn(a, b):
    return lax.dot_general(a, b, (((0,), (0,)), ((), ())), preferred_element_type=F32)


def rows_of(shape):
    return lax.broadcasted_iota(jnp.int32, shape, 0)


def cols_of(shape):
    return lax.broadcasted_iota(jnp.int32, shape, 1)


def divided(n, by):
    return ((n.astype(F32) + 0.5) * (1.0 / by)).astype(jnp.int32)


def picked(mask):
    return mask.astype(F32).astype(BF)


def dispatch_kernel(experts, cap, share_ref, routes_ref, gates_ref, tok0, tok1, cot0, cot1, send_ref, rank_ref):
    toks = routes_ref.shape[1]
    block = 4 * cap
    route = [routes_ref[k : k + 1, :] for k in range(2)]
    ids = rows_of((experts, toks))
    named = [ids == r for r in route]
    both = picked(named[0] | named[1])
    before = picked(rows_of((toks, toks)) < cols_of((toks, toks)))
    earlier = nn(both, before)
    ranks = [jnp.sum(jnp.where(m, earlier, 0.0), axis=0, keepdims=True).astype(jnp.int32) for m in named]
    rank_ref[...] = jnp.concatenate(ranks, axis=0)
    slot = rows_of((experts * block, toks))
    first = [r * block + k for r, k in zip(route, ranks)]
    rows_x = jnp.zeros((experts * block, LANES), F32)
    rows_c = rows_x
    gate = jnp.zeros((experts * block, toks), F32)
    for n, (tok, cot) in enumerate(((tok0, cot0), (tok1, cot1))):
        at = [slot == f + 2 * n * cap for f in first]
        rows_x = rows_x + nn(picked(at[0] | at[1]), tok[...])
        at = [slot == f + (2 * n + 1) * cap for f in first]
        rows_c = rows_c + nn(picked(at[0] | at[1]), cot[...])
        for k in range(2):
            gate = jnp.where(at[k], gates_ref[k : k + 1, :], gate)
    gate = jnp.sum(gate, axis=1, keepdims=True)
    send_ref[...] = (rows_x + gate * rows_c).astype(BF)


def compact_kernel(cap, recv_ref, out_ref):
    experts = recv_ref.shape[0] // (4 * cap)
    slots = experts * cap
    group = 8 if experts % 8 == 0 else experts
    size, count = 4 * cap * group, cap * group
    row, at = rows_of((size, size)), cols_of((size, size))
    kind = divided(row, count)
    row = row - kind * count
    source = divided(row, cap)
    order = picked(at == source * (3 * cap) + row + kind * cap)
    for g in range(experts // group):
        rows = nn(order, recv_ref[g * size : (g + 1) * size, :]).astype(BF)
        for n in range(4):
            out_ref[n * slots + g * count : n * slots + (g + 1) * count, :] = rows[n * count : (n + 1) * count, :]


def swiglu_back(x, c, gate_weight, up_weight, down_weight):
    pre_gate = nt(gate_weight, x)
    pre_up = nt(up_weight, x)
    hidden_grad = nt(down_weight, c)
    s = jax.nn.sigmoid(pre_gate)
    activated = pre_gate * s
    hidden = (activated * pre_up).astype(BF)
    d_gate = (hidden_grad * pre_up * s * (1.0 + pre_gate * (1.0 - s))).astype(BF)
    d_up = (hidden_grad * activated).astype(BF)
    return hidden, hidden_grad, d_gate, d_up


def shared_kernel(tok_ref, cot_ref, gate_ref, up_ref, down_ref, piece_ref, term_ref, lined_ref):
    tok, cot = tok_ref[...], cot_ref[...]
    gate_weight, up_weight = gate_ref[...], up_ref[...]
    hidden, _, d_gate, d_up = swiglu_back(tok, cot, gate_weight, up_weight, down_ref[...])
    back = tn(
        jnp.concatenate([d_gate, d_up], axis=0), jnp.concatenate([gate_weight, up_weight], axis=0)
    ).astype(BF)
    term = nn(hidden, cot)
    for p in range(piece_ref.shape[0]):
        piece_ref[p] = back[:, p * LANES : (p + 1) * LANES]
        lined_ref[:, p, :] = term[:, p * LANES : (p + 1) * LANES]
    term_ref[...] = lined_ref[...].reshape(term_ref.shape).astype(BF)


OFFSETS = (0, 4, 7, 3, 1, 5, 6, 2)


def assemble(at_ref, own_ref, other_ref, x_ref, c_ref):
    slots = c_ref.shape[0]
    y, core = at_ref[0], at_ref[1]
    for n, offset in enumerate(OFFSETS):
        chip = lax.rem(y + offset, len(OFFSETS))
        for ref, side in ((own_ref, core), (other_ref, 1 - core)):
            lane = pl.multiple_of((2 * chip + side) * LANES, LANES)
            if x_ref is not None:
                x_ref[:, pl.ds(lane, LANES)] = ref[n, 0:slots, :]
            c_ref[:, pl.ds(lane, LANES)] = ref[n, slots : 2 * slots, :]


def expert_kernel(
    extra, at_ref, own_ref, other_ref, gate_ref, up_ref, down_ref, piece_ref,
    keep_ref, send_ref, hidden_ref, g_gate_ref, g_up_ref, x_ref, c_ref, blocks_ref,
):
    assemble(at_ref, own_ref, other_ref, x_ref, c_ref)
    slots = x_ref.shape[0]
    shares, toks, _ = piece_ref.shape
    gate_weight, up_weight = gate_ref[...], up_ref[...]
    hidden, hidden_grad, d_gate, d_up = swiglu_back(
        x_ref[...], c_ref[...], gate_weight, up_weight, down_ref[...]
    )
    hidden_ref[...] = hidden
    dots = jnp.sum(hidden.astype(F32) * hidden_grad, axis=0, keepdims=True)
    back = tn(
        jnp.concatenate([d_gate, d_up], axis=0), jnp.concatenate([gate_weight, up_weight], axis=0)
    ).astype(BF)
    for p in range(shares):
        blocks_ref[p] = back[:, p * LANES : (p + 1) * LANES]
    line = rows_of((extra, LANES))
    rest = jnp.zeros((extra, LANES), F32)
    for k, (d, out_ref) in enumerate(((d_gate, g_gate_ref), (d_up, g_up_ref))):
        g = nn(d, x_ref[...])
        out_ref[...] = g
        sums = jnp.sum(g * g, axis=0, keepdims=True)
        for p in range(shares):
            rest = jnp.where(line == k * shares + p, sums[:, p * LANES : (p + 1) * LANES], rest)
    wide = up(slots, LANES)
    dots = jnp.concatenate([dots, jnp.zeros((1, wide - slots), F32)], axis=1)
    for k in range(wide // LANES):
        rest = jnp.where(line == 2 * shares + k, dots[:, k * LANES : (k + 1) * LANES], rest)
    rest = rest.astype(BF)
    core = at_ref[1]
    for y in range(keep_ref.shape[0]):
        for ref, side in ((keep_ref, core), (send_ref, 1 - core)):
            ref[y, 0:slots, :] = blocks_ref[2 * y + side]
            ref[y, slots : slots + toks, :] = piece_ref[2 * y + side]
            ref[y, slots + toks : slots + toks + extra, :] = rest


def down_kernel(at_ref, own_ref, other_ref, hidden_ref, g_down_ref, n_down_ref, c_ref):
    assemble(at_ref, own_ref, other_ref, None, c_ref)
    g_down = nn(hidden_ref[...], c_ref[...])
    g_down_ref[...] = g_down
    n_down_ref[...] = jnp.sum(g_down * g_down, axis=1, keepdims=True) * (1.0 / g_down.shape[1])


def return_kernel(cap, block, width, parts_ref, back_ref, shared_ref, norm_ref):
    size = back_ref.shape[0]
    slots = size // block * cap
    toks = shared_ref.shape[0]
    shares = norm_ref.shape[1] // LANES
    total = parts_ref[0].astype(F32)
    for y in range(1, parts_ref.shape[0]):
        total = total + parts_ref[y].astype(F32)
    shared_ref[...] = total[slots : slots + toks, :]
    for k in range(2):
        for p in range(shares):
            at = slots + toks + k * shares + p
            norm_ref[k : k + 1, p * LANES : (p + 1) * LANES] = total[at : at + 1, :] * (1.0 / width)
    row = rows_of((size, slots))
    slot = cols_of((size, slots))
    source = divided(row, block)
    inner = row - source * block
    mask = (slot == source * cap + inner) & (inner < cap)
    back = nn(picked(mask), total[0:slots, :].astype(BF))
    row = rows_of((size, LANES))
    source = divided(row, block)
    is_dot = row == source * block + cap
    for k in range(up(slots, LANES) // LANES):
        at = slots + toks + 2 * shares + k
        dots = total[at : at + 1, :].astype(BF).astype(F32)
        mine = divided(cols_of((size, LANES)) + k * LANES, cap) == source
        left = jnp.where(is_dot & mine, dots, 0.0).astype(BF)
        number = rows_of((LANES, LANES)) + k * LANES
        place = number - divided(number, cap) * cap
        back = back + nn(left, picked(place == cols_of((LANES, LANES))))
    back_ref[...] = back.astype(BF)


def combine_kernel(cap, block, recv_ref, routes_ref, rank_ref, gates_ref, shared_ref, grad_ref, gate_grad_ref):
    size = recv_ref.shape[0]
    toks = routes_ref.shape[1]
    recv = recv_ref[...]
    row = rows_of((size, toks))
    lane = rows_of((LANES, toks))
    at = []
    for k in range(2):
        route, rank = routes_ref[k : k + 1, :], rank_ref[k : k + 1, :]
        at.append(row == route * block + rank)
        dots = tn(recv, picked(row == route * block + cap))
        dot = jnp.sum(jnp.where(lane == rank, dots, 0.0), axis=0, keepdims=True)
        gate_grad_ref[k : k + 1, :] = dot / gates_ref[k : k + 1, :]
    grad_ref[...] = (tn(picked(at[0] | at[1]), recv) + shared_ref[...]).astype(BF)


def local(body, args, outs, scratch=(), scalars=0, flops=0):
    specs = [pl.BlockSpec(memory_space=pltpu.SMEM)] * scalars
    specs = specs + [pl.BlockSpec(memory_space=pltpu.VMEM)] * (len(args) - scalars)
    return pl.pallas_call(
        body,
        in_specs=specs,
        out_shape=tuple(jax.ShapeDtypeStruct(s, d) for s, d in outs),
        out_specs=tuple(pl.BlockSpec(memory_space=pltpu.VMEM) for _ in outs),
        scratch_shapes=list(scratch),
        cost_estimate=pl.CostEstimate(flops=flops, bytes_accessed=flops // 1000, transcendentals=0),
        compiler_params=pltpu.CompilerParams(vmem_limit_bytes=40 * 1024 * 1024),
    )(*args)


def shifted(x, by, count):
    return lax.ppermute(x, "y", [(i, (i + by) % count) for i in range(count)])


def all_steps(tokens, routes, route_gates, cotangent, w_gate, w_up, w_down, s_gate, s_up, s_down):
    tp = ("y", "core")
    ep_count = lax.axis_size("ep")
    shares = lax.axis_size(tp)
    chips = shares // 2
    y = lax.axis_index("y").astype(jnp.int32)
    core = lax.axis_index("core").astype(jnp.int32)
    at = jnp.stack([y, core])
    share = jnp.stack([2 * y + core, 2 * ((y + chips // 2) % chips) + core])
    toks, width = tokens.shape
    units = w_gate.shape[2]
    cap = max(2, (9 * toks * 2 + 8 * ep_count - 1) // (8 * ep_count))
    slots = ep_count * cap
    back_block = up(cap + 1, 8)
    routes_t, gates_t = routes.T, route_gates.T

    narrow = [pl.BlockSpec((toks, LANES), lambda i, s, n=n: (0, s[n])) for n in range(2)]
    whole = pl.BlockSpec((2, toks), lambda i, s: (0, 0))
    send, ranks = pl.pallas_call(
        functools.partial(dispatch_kernel, ep_count, cap),
        out_shape=(
            jax.ShapeDtypeStruct((4 * slots, LANES), BF),
            jax.ShapeDtypeStruct((2, toks), jnp.int32),
        ),
        grid_spec=pltpu.PrefetchScalarGridSpec(
            num_scalar_prefetch=1,
            grid=(1,),
            in_specs=[whole, whole] + narrow + narrow,
            out_specs=(
                pl.BlockSpec((4 * slots, LANES), lambda i, s: (0, 0)),
                pl.BlockSpec((2, toks), lambda i, s: (0, 0)),
            ),
        ),
    )(share, routes_t, gates_t, tokens, tokens, cotangent, cotangent)
    recv = lax.all_to_all(send.reshape(ep_count, 4 * cap, LANES), "ep", 0, 0, tiled=True)

    piece, term = local(
        shared_kernel,
        (tokens, cotangent, s_gate.T, s_up.T, s_down),
        [((shares, toks, LANES), BF), ((ep_count, units * shares // ep_count, LANES), BF)],
        [pltpu.VMEM((units, shares, LANES), F32)],
        flops=4 * 10**9,
    )
    recv, piece, term = lax.optimization_barrier((recv, piece, term))
    term_parts = lax.all_to_all(term, "ep", 0, 0, tiled=True)

    (mine,) = local(
        functools.partial(compact_kernel, cap), (recv.reshape(4 * slots, LANES),), [((4 * slots, LANES), BF)]
    )
    mine = mine.reshape(2, 2 * slots, LANES)
    near = [shifted(mine, 1, chips), shifted(mine, -1, chips)]
    near.append(shifted(mine[:1], 2, chips))
    near.append(shifted(mine[:1], -2, chips))
    own = jnp.concatenate([mine] + near, axis=0)
    swap = [(0, 1), (1, 0)]
    other = lax.ppermute(own, "core", swap)

    extra = up(2 * shares + up(slots, LANES) // LANES, 16)
    wide = pltpu.VMEM((slots, width), BF)
    moved = ((chips, slots + toks + extra, LANES), BF)
    grads = ((units, width), F32)
    keep, give, hidden, g_gate, g_up = local(
        functools.partial(expert_kernel, extra),
        (at, own, other, w_gate[0].T, w_up[0].T, w_down[0], piece),
        [moved, moved, ((units, slots), BF), grads, grads],
        [wide, wide, pltpu.VMEM((shares, slots, LANES), BF)],
        scalars=1,
        flops=8 * 10**9,
    )
    taken = lax.ppermute(give, "core", swap)
    pair = (keep.astype(F32) + taken.astype(F32)).astype(BF)
    pair_parts = lax.all_to_all(pair, "y", 0, 0, tiled=True)
    g_down, n_down = local(
        down_kernel, (at, own, other, hidden), [grads, ((units, 1), F32)], [wide], scalars=1, flops=3 * 10**9
    )

    back, shared_back, norm_in = local(
        functools.partial(return_kernel, cap, back_block, units * shares),
        (pair_parts,),
        [((ep_count * back_block, LANES), BF), ((toks, LANES), F32), ((2, width), F32)],
    )
    came = lax.all_to_all(back.reshape(ep_count, back_block, LANES), "ep", 0, 0, tiled=True)
    token_grad, gate_grad = local(
        functools.partial(combine_kernel, cap, back_block),
        (came.reshape(ep_count * back_block, LANES), routes_t, ranks, gates_t, shared_back),
        [((toks, LANES), BF), ((2, toks), F32)],
    )

    grad_shared = jnp.sum(term_parts.astype(F32), axis=0).reshape(-1, width)
    norm_shared = jnp.mean(grad_shared**2, axis=1)
    return (
        token_grad,
        gate_grad.T,
        g_gate.T[None],
        g_up.T[None],
        g_down[None],
        grad_shared,
        norm_in[None],
        n_down.reshape(1, units),
        norm_shared,
    )


def solution(mesh):
    tp = ("y", "core")
    ep_count, tp_count = mesh.devices.shape
    fine = Mesh(mesh.devices.reshape(ep_count, tp_count // 2, 2), ("ep", "y", "core"))
    placed = (
        P("ep", None),
        P("ep", None),
        P("ep", None),
        P("ep", None),
        P("ep", None, tp),
        P("ep", None, tp),
        P("ep", tp, None),
        P(None, tp),
        P(None, tp),
        P(tp, None),
    )
    return jax.shard_map(
        all_steps,
        mesh=fine,
        in_specs=placed,
        out_specs=(
            P("ep", tp),
            P("ep", None),
            P("ep", None, tp),
            P("ep", None, tp),
            P("ep", tp, None),
            P(("y", "core", "ep"), None),
            P("ep", None, None),
            P("ep", tp),
            P(("y", "core", "ep")),
        ),
        check_vma=False,
    )
```

```python
import functools

import jax
import jax.numpy as jnp
from jax import lax
from jax.experimental import pallas as pl
from jax.experimental.pallas import tpu as pltpu
from jax.sharding import Mesh, PartitionSpec as P

BF = jnp.bfloat16
F32 = jnp.float32
LANES = 128


def up(n, k):
    return -(-n // k) * k


def nn(a, b):
    return lax.dot_general(a, b, (((1,), (0,)), ((), ())), preferred_element_type=F32)


def nt(a, b):
    return lax.dot_general(a, b, (((1,), (1,)), ((), ())), preferred_element_type=F32)


def tn(a, b):
    return lax.dot_general(a, b, (((0,), (0,)), ((), ())), preferred_element_type=F32)


def rows_of(shape):
    return lax.broadcasted_iota(jnp.int32, shape, 0)


def cols_of(shape):
    return lax.broadcasted_iota(jnp.int32, shape, 1)


def divided(n, by):
    return ((n.astype(F32) + 0.5) * (1.0 / by)).astype(jnp.int32)


def picked(mask):
    return mask.astype(F32).astype(BF)


def groups_of(experts):
    return 8 if experts % 8 == 0 else experts


def regroup(cap, group, to_kinds):
    size, count = 4 * cap * group, cap * group
    kinds, sources = rows_of((size, size)), cols_of((size, size))
    if not to_kinds:
        kinds, sources = sources, kinds
    kind = divided(kinds, count)
    kinds = kinds - kind * count
    source = divided(kinds, cap)
    return picked(sources == source * (3 * cap) + kinds + kind * cap)


def dispatch_kernel(experts, cap, share_ref, routes_ref, gates_ref, tok0, tok1, cot0, cot1, send_ref, rank_ref):
    toks = routes_ref.shape[1]
    slots = experts * cap
    route = [routes_ref[k : k + 1, :] for k in range(2)]
    ids = rows_of((experts, toks))
    named = [ids == r for r in route]
    both = picked(named[0] | named[1])
    before = picked(rows_of((toks, toks)) < cols_of((toks, toks)))
    earlier = nn(both, before)
    ranks = [jnp.sum(jnp.where(m, earlier, 0.0), axis=0, keepdims=True).astype(jnp.int32) for m in named]
    rank_ref[...] = jnp.concatenate(ranks, axis=0)
    slot = rows_of((slots, toks))
    same = rows_of((toks, toks)) == cols_of((toks, toks))
    toks_both = jnp.concatenate([tok0[...], tok1[...]], axis=1)
    cots_both = jnp.concatenate([cot0[...], cot1[...]], axis=1).astype(F32)
    rows_x = rows_c = None
    for k in range(2):
        at = picked(slot == route[k] * cap + ranks[k])
        gate = jnp.sum(jnp.where(same, gates_ref[k : k + 1, :], 0.0), axis=1, keepdims=True)
        x, c = nn(at, toks_both), nn(at, (gate * cots_both).astype(BF))
        rows_x, rows_c = (x, c) if rows_x is None else (rows_x + x, rows_c + c)
    rows_x, rows_c = rows_x.astype(BF), rows_c.astype(BF)
    group = groups_of(experts)
    order = regroup(cap, group, False)
    size, count = 4 * cap * group, cap * group
    for g in range(experts // group):
        rows = slice(g * count, (g + 1) * count)
        kinds = [m[rows, n * LANES : (n + 1) * LANES] for n in range(2) for m in (rows_x, rows_c)]
        send_ref[g * size : (g + 1) * size, :] = nn(order, jnp.concatenate(kinds, axis=0)).astype(BF)


def compact_kernel(cap, recv_ref, keep_ref, taken_ref, up_ref, down_ref, far_up_ref, far_down_ref, stay_ref):
    experts = recv_ref.shape[0] // (4 * cap)
    slots = experts * cap
    toks = keep_ref.shape[1]
    group = groups_of(experts)
    size, count = 4 * cap * group, cap * group
    order = regroup(cap, group, True)
    for g in range(experts // group):
        rows = nn(order, recv_ref[g * size : (g + 1) * size, :]).astype(BF)
        for n in range(4):
            at = slice(n * slots + g * count, n * slots + (g + 1) * count)
            part = rows[n * count : (n + 1) * count, :]
            up_ref[at, :] = part
            down_ref[at, :] = part
            if n < 2:
                far_up_ref[at, :] = part
                far_down_ref[at, :] = part
    near, far = 4 * slots, 2 * slots
    for n, (ref, at) in enumerate(
        ((up_ref, near), (up_ref, near + toks), (down_ref, near), (down_ref, near + toks), (far_up_ref, far), (far_down_ref, far))
    ):
        ref[at : at + toks, :] = (keep_ref[n].astype(F32) + taken_ref[n].astype(F32)).astype(BF)
    for n in range(2):
        stay_ref[n] = keep_ref[6 + n].astype(F32) + taken_ref[6 + n].astype(F32)


def join_kernel(mine_ref, up_ref, down_ref, far_up_ref, far_down_ref, stay_ref, own_ref, near_ref, far_ref):
    rows = own_ref.shape[1]
    toks = near_ref.shape[0]
    at = 0
    for ref, count in ((mine_ref, 2), (up_ref, 2), (down_ref, 2), (far_up_ref, 1), (far_down_ref, 1)):
        for n in range(count):
            own_ref[at] = ref[n * rows : (n + 1) * rows, :]
            at += 1
    near = stay_ref[0]
    for ref, count in ((up_ref, 2), (down_ref, 2), (far_up_ref, 1), (far_down_ref, 1)):
        near = near + ref[count * rows : count * rows + toks, :].astype(F32)
    near_ref[...] = near
    far = stay_ref[1]
    for ref in (up_ref, down_ref):
        far = far + ref[2 * rows + toks : 2 * rows + 2 * toks, :].astype(F32)
    far_ref[...] = far.astype(BF)


def swiglu_back(x, c, gate_weight, up_weight, down_weight):
    pre_gate = nt(gate_weight, x)
    pre_up = nt(up_weight, x)
    hidden_grad = nt(down_weight, c)
    s = jax.nn.sigmoid(pre_gate)
    activated = pre_gate * s
    hidden = (activated * pre_up).astype(BF)
    d_gate = (hidden_grad * pre_up * s * (1.0 + pre_gate * (1.0 - s))).astype(BF)
    d_up = (hidden_grad * activated).astype(BF)
    return hidden, hidden_grad, d_gate, d_up


ORDER = (1, 5, 7, 3, 2, 6, 0, 4)


def shared_kernel(
    at_ref, tok_ref, cot_ref, gate_ref, up_ref, down_ref, keep_ref, send_ref, term_ref, lined_ref, blocks_ref
):
    tok, cot = tok_ref[...], cot_ref[...]
    gate_weight, up_weight = gate_ref[...], up_ref[...]
    hidden, _, d_gate, d_up = swiglu_back(tok, cot, gate_weight, up_weight, down_ref[...])
    back = tn(
        jnp.concatenate([d_gate, d_up], axis=0), jnp.concatenate([gate_weight, up_weight], axis=0)
    ).astype(BF)
    term = nn(hidden, cot)
    for p in range(blocks_ref.shape[0]):
        blocks_ref[p] = back[:, p * LANES : (p + 1) * LANES]
        lined_ref[:, p, :] = term[:, p * LANES : (p + 1) * LANES]
    term_ref[...] = lined_ref[...].reshape(term_ref.shape).astype(BF)
    y, core = at_ref[0] >> 1, at_ref[0] & 1
    for n, offset in enumerate(ORDER):
        chip = lax.rem(y + offset, len(ORDER))
        keep_ref[n] = blocks_ref[2 * chip + core]
        send_ref[n] = blocks_ref[2 * chip + 1 - core]


OFFSETS = (0, 4, 7, 3, 1, 5, 6, 2)


def assemble(at_ref, own_ref, other_ref, x_ref, c_ref):
    slots = c_ref.shape[0]
    y, core = at_ref[0] >> 1, at_ref[0] & 1
    for n, offset in enumerate(OFFSETS):
        chip = lax.rem(y + offset, len(OFFSETS))
        for ref, side in ((own_ref, core), (other_ref, 1 - core)):
            lane = pl.multiple_of((2 * chip + side) * LANES, LANES)
            if x_ref is not None:
                x_ref[:, pl.ds(lane, LANES)] = ref[n, 0:slots, :]
            c_ref[:, pl.ds(lane, LANES)] = ref[n, slots : 2 * slots, :]


def lanes_of(refs, side, out_ref):
    at = 0
    for ref in refs:
        rows = ref.shape[0]
        for y in range(ref.shape[1] // (2 * LANES)):
            lane = pl.multiple_of((2 * y + side) * LANES, LANES)
            out_ref[at : at + rows, y * LANES : (y + 1) * LANES] = ref[:, pl.ds(lane, LANES)]
        at += rows


def expert_kernel(
    extra, at_ref, own_ref, other_ref, gate_ref, up_ref, down_ref,
    send_ref, dots_ref, hidden_ref, joined_ref, x_ref, c_ref, half_ref,
):
    assemble(at_ref, own_ref, other_ref, x_ref, c_ref)
    slots = x_ref.shape[0]
    hidden, hidden_grad, d_gate, d_up = swiglu_back(
        x_ref[...], c_ref[...], gate_ref[...], up_ref[...], down_ref[...]
    )
    hidden_ref[...] = hidden
    joined = jnp.concatenate([d_gate, d_up], axis=0)
    joined_ref[...] = joined
    lanes_of((gate_ref, up_ref), 1 - (at_ref[0] & 1), half_ref)
    back = tn(joined, half_ref[...]).astype(BF)
    dots = jnp.sum(hidden.astype(F32) * hidden_grad, axis=0, keepdims=True)
    wide = up(slots, LANES)
    dots = jnp.concatenate([dots, jnp.zeros((1, wide - slots), F32)], axis=1)
    line = rows_of((extra, LANES))
    rest = jnp.zeros((extra, LANES), F32)
    for k in range(wide // LANES):
        rest = jnp.where(line == k, dots[:, k * LANES : (k + 1) * LANES], rest)
    rest = rest.astype(BF)
    dots_ref[...] = rest
    for y in range(send_ref.shape[0]):
        send_ref[y, 0:slots, :] = back[:, y * LANES : (y + 1) * LANES]
        send_ref[y, slots : slots + extra, :] = rest


def keep_kernel(at_ref, x_ref, joined_ref, gate_ref, up_ref, keep_ref, g_gate_ref, g_up_ref, squares_ref, half_ref):
    units, width = g_gate_ref.shape
    shares = width // LANES
    joined = joined_ref[...]
    lanes_of((gate_ref, up_ref), at_ref[0] & 1, half_ref)
    back = tn(joined, half_ref[...]).astype(BF)
    for y in range(keep_ref.shape[0]):
        keep_ref[y] = back[:, y * LANES : (y + 1) * LANES]
    line = rows_of((2 * shares, LANES))
    rest = jnp.zeros((2 * shares, LANES), F32)
    for k, out_ref in enumerate((g_gate_ref, g_up_ref)):
        g = nn(joined[k * units : (k + 1) * units, :], x_ref[...])
        out_ref[...] = g
        sums = jnp.sum(g * g, axis=0, keepdims=True)
        for p in range(shares):
            rest = jnp.where(line == k * shares + p, sums[:, p * LANES : (p + 1) * LANES], rest)
    squares_ref[...] = rest.astype(BF)


def add_kernel(keep_ref, taken_ref, dots_ref, squares_ref, out_ref):
    slots = keep_ref.shape[1]
    rows = taken_ref.shape[1]
    dots, squares = dots_ref[...].astype(F32), squares_ref[...]
    for y in range(out_ref.shape[0]):
        out_ref[y, 0:slots, :] = (keep_ref[y].astype(F32) + taken_ref[y, 0:slots, :].astype(F32)).astype(BF)
        out_ref[y, slots:rows, :] = (dots + taken_ref[y, slots:rows, :].astype(F32)).astype(BF)
        out_ref[y, rows : rows + squares.shape[0], :] = squares


def down_kernel(at_ref, own_ref, other_ref, hidden_ref, g_down_ref, n_down_ref, c_ref):
    assemble(at_ref, own_ref, other_ref, None, c_ref)
    g_down = nn(hidden_ref[...], c_ref[...])
    g_down_ref[...] = g_down
    units = g_down.shape[0]
    n_down = jnp.sum(g_down * g_down, axis=1, keepdims=True) * (1.0 / g_down.shape[1])
    same = rows_of((units, units)) == cols_of((units, units))
    n_down_ref[...] = jnp.sum(jnp.where(same, n_down, 0.0), axis=0, keepdims=True)


def return_kernel(cap, block, parts_ref, back_ref, squares_ref):
    size = back_ref.shape[0]
    slots = size // block * cap
    total = parts_ref[0].astype(F32)
    for y in range(1, parts_ref.shape[0]):
        total = total + parts_ref[y].astype(F32)
    squares_ref[...] = total[total.shape[0] - squares_ref.shape[0] :, :]
    row = rows_of((size, slots))
    slot = cols_of((size, slots))
    source = divided(row, block)
    inner = row - source * block
    mask = (slot == source * cap + inner) & (inner < cap)
    back = nn(picked(mask), total[0:slots, :].astype(BF))
    row = rows_of((size, LANES))
    source = divided(row, block)
    is_dot = row == source * block + cap
    for k in range(up(slots, LANES) // LANES):
        dots = total[slots + k : slots + k + 1, :].astype(BF).astype(F32)
        mine = divided(cols_of((size, LANES)) + k * LANES, cap) == source
        left = jnp.where(is_dot & mine, dots, 0.0).astype(BF)
        number = rows_of((LANES, LANES)) + k * LANES
        place = number - divided(number, cap) * cap
        back = back + nn(left, picked(place == cols_of((LANES, LANES))))
    back_ref[...] = back.astype(BF)


def shared_sum_kernel(parts_ref, grad_ref, norm_ref):
    total = parts_ref[0].astype(F32)
    for e in range(1, parts_ref.shape[0]):
        total = total + parts_ref[e].astype(F32)
    rows, width = grad_ref.shape
    count = width // LANES
    lane = cols_of(norm_ref.shape)
    norm = jnp.zeros(norm_ref.shape, F32)
    for i in range(rows):
        mine = total[i * count : (i + 1) * count, :]
        for p in range(count):
            grad_ref[i : i + 1, p * LANES : (p + 1) * LANES] = mine[p : p + 1, :]
        square = jnp.sum(jnp.sum(mine * mine, axis=0, keepdims=True), axis=1, keepdims=True)
        norm = jnp.where(lane == i, square * (1.0 / width), norm)
    norm_ref[...] = norm


def combine_kernel(cap, block, recv_ref, routes_ref, rank_ref, gates_ref, near_ref, far_ref, grad_ref, gate_grad_ref):
    size = recv_ref.shape[0]
    toks = routes_ref.shape[1]
    recv = recv_ref[...]
    row = rows_of((size, toks))
    lane = rows_of((LANES, toks))
    at = []
    for k in range(2):
        route, rank = routes_ref[k : k + 1, :], rank_ref[k : k + 1, :]
        at.append(row == route * block + rank)
        dots = tn(recv, picked(row == route * block + cap))
        dot = jnp.sum(jnp.where(lane == rank, dots, 0.0), axis=0, keepdims=True)
        gate_grad_ref[k : k + 1, :] = dot / gates_ref[k : k + 1, :]
    grad_ref[...] = (tn(picked(at[0] | at[1]), recv) + (near_ref[...] + far_ref[...].astype(F32))).astype(BF)


def local(body, args, outs, scratch=(), scalars=0, flops=2 * 10**9):
    specs = [pl.BlockSpec(memory_space=pltpu.SMEM)] * scalars
    specs = specs + [pl.BlockSpec(memory_space=pltpu.VMEM)] * (len(args) - scalars)
    return pl.pallas_call(
        body,
        in_specs=specs,
        out_shape=tuple(jax.ShapeDtypeStruct(s, d) for s, d in outs),
        out_specs=tuple(pl.BlockSpec(memory_space=pltpu.VMEM) for _ in outs),
        scratch_shapes=list(scratch),
        cost_estimate=pl.CostEstimate(flops=flops, bytes_accessed=flops // 500, transcendentals=0),
        compiler_params=pltpu.CompilerParams(vmem_limit_bytes=20 * 1024 * 1024),
    )(*args)


def shifted(x, by, count):
    return lax.ppermute(x, "y", [(i, (i + by) % count) for i in range(count)])


def all_steps(tokens, routes, route_gates, cotangent, w_gate, w_up, w_down, s_gate, s_up, s_down):
    tp = ("y", "core")
    ep_count = lax.axis_size("ep")
    shares = lax.axis_size(tp)
    chips = shares // 2
    at = lax.axis_index(tp).astype(jnp.int32).reshape(1)
    toks, width = tokens.shape
    units = w_gate.shape[2]
    cap = max(2, (9 * toks * 2 + 8 * ep_count - 1) // (8 * ep_count))
    slots = ep_count * cap
    back_block = up(cap + 1, 8)
    routes_t, gates_t = routes.T, route_gates.T

    narrow = [pl.BlockSpec((toks, LANES), lambda i, s, n=n: (0, lax.rem(s[0] + n * chips, shares))) for n in range(2)]
    whole = pl.BlockSpec((2, toks), lambda i, s: (0, 0))
    send, ranks = pl.pallas_call(
        functools.partial(dispatch_kernel, ep_count, cap),
        out_shape=(
            jax.ShapeDtypeStruct((4 * slots, LANES), BF),
            jax.ShapeDtypeStruct((2, toks), jnp.int32),
        ),
        grid_spec=pltpu.PrefetchScalarGridSpec(
            num_scalar_prefetch=1,
            grid=(1,),
            in_specs=[whole, whole] + narrow + narrow,
            out_specs=(
                pl.BlockSpec((4 * slots, LANES), lambda i, s: (0, 0)),
                pl.BlockSpec((2, toks), lambda i, s: (0, 0)),
            ),
        ),
    )(at, routes_t, gates_t, tokens, tokens, cotangent, cotangent)
    recv = lax.all_to_all(send.reshape(ep_count, 4 * cap, LANES), "ep", 0, 0, tiled=True)

    keep, give, term = local(
        shared_kernel,
        (at, tokens, cotangent, s_gate.T, s_up.T, s_down),
        [((chips, toks, LANES), BF)] * 2 + [((ep_count, units * shares // ep_count, LANES), BF)],
        [pltpu.VMEM((units, shares, LANES), F32), pltpu.VMEM((shares, toks, LANES), BF)],
        scalars=1,
        flops=4 * 10**9,
    )
    swap = [(0, 1), (1, 0)]
    taken = lax.ppermute(give, "core", swap)
    recv, keep, taken, term = lax.optimization_barrier((recv, keep, taken, term))
    term_parts = lax.all_to_all(term, "ep", 0, 0, tiled=True)

    near, far = 4 * slots, 2 * slots
    go_up, go_down, go_far_up, go_far_down, stay = local(
        functools.partial(compact_kernel, cap),
        (recv.reshape(4 * slots, LANES), keep, taken),
        [((near + 2 * toks, LANES), BF)] * 2 + [((far + toks, LANES), BF)] * 2 + [((2, toks, LANES), F32)],
    )
    came_up = shifted(go_up, 1, chips)
    came_down = shifted(go_down, -1, chips)
    came_far_up = shifted(go_far_up, 2, chips)
    came_far_down = shifted(go_far_down, -2, chips)
    own, shared_near, shared_far = local(
        join_kernel,
        (go_up, came_up, came_down, came_far_up, came_far_down, stay),
        [((chips, far, LANES), BF), ((toks, LANES), F32), ((toks, LANES), BF)],
    )
    other = lax.ppermute(own, "core", swap)
    shared_far = shifted(shared_far, chips // 2, chips)

    extra = up(up(slots, LANES) // LANES, 16)
    weights = (w_gate[0].T, w_up[0].T)
    half = pltpu.VMEM((2 * units, width // 2), BF)
    give, dots, hidden, joined, x = local(
        functools.partial(expert_kernel, extra),
        (at, own, other, *weights, w_down[0]),
        [
            ((chips, slots + extra, LANES), BF),
            ((extra, LANES), BF),
            ((units, slots), BF),
            ((2 * units, slots), BF),
            ((slots, width), BF),
        ],
        [pltpu.VMEM((slots, width), BF), half],
        scalars=1,
        flops=6 * 10**9,
    )
    taken = lax.ppermute(give, "core", swap)
    grads = ((units, width), F32)
    keep, g_gate, g_up, squares = local(
        keep_kernel,
        (at, x, joined, *weights),
        [((chips, slots, LANES), BF), grads, grads, ((2 * shares, LANES), BF)],
        [half],
        scalars=1,
        flops=4 * 10**9,
    )
    (pair,) = local(
        add_kernel, (keep, taken, dots, squares), [((chips, slots + extra + 2 * shares, LANES), BF)]
    )
    pair_parts = lax.all_to_all(pair, "y", 0, 0, tiled=True)

    g_down, n_down = local(
        down_kernel,
        (at, own, other, hidden),
        [grads, ((1, units), F32)],
        [pltpu.VMEM((slots, width), BF)],
        scalars=1,
        flops=3 * 10**9,
    )
    back, squares = local(
        functools.partial(return_kernel, cap, back_block),
        (pair_parts,),
        [((ep_count * back_block, LANES), BF), ((2 * shares, LANES), F32)],
    )
    squares = squares + lax.ppermute(squares, "core", swap)
    norm_in = (squares * (1.0 / (units * shares))).reshape(2, width)
    came = lax.all_to_all(back.reshape(ep_count, back_block, LANES), "ep", 0, 0, tiled=True)
    token_grad, gate_grad = local(
        functools.partial(combine_kernel, cap, back_block),
        (came.reshape(ep_count * back_block, LANES), routes_t, ranks, gates_t, shared_near, shared_far),
        [((toks, LANES), BF), ((2, toks), F32)],
    )

    grad_shared, norm_shared = local(
        shared_sum_kernel, (term_parts,), [((term.shape[1] * LANES // width, width), F32), ((1, LANES), F32)]
    )
    norm_shared = norm_shared[0, : grad_shared.shape[0]]
    return (
        token_grad,
        gate_grad.T,
        g_gate.T[None],
        g_up.T[None],
        g_down[None],
        grad_shared,
        norm_in[None],
        n_down,
        norm_shared,
    )


def solution(mesh):
    tp = ("y", "core")
    ep_count, tp_count = mesh.devices.shape
    fine = Mesh(mesh.devices.reshape(ep_count, tp_count // 2, 2), ("ep", "y", "core"))
    placed = (
        P("ep", None),
        P("ep", None),
        P("ep", None),
        P("ep", None),
        P("ep", None, tp),
        P("ep", None, tp),
        P("ep", tp, None),
        P(None, tp),
        P(None, tp),
        P(tp, None),
    )
    return jax.shard_map(
        all_steps,
        mesh=fine,
        in_specs=placed,
        out_specs=(
            P("ep", tp),
            P("ep", None),
            P("ep", None, tp),
            P("ep", None, tp),
            P("ep", tp, None),
            P(("y", "core", "ep"), None),
            P("ep", None, None),
            P("ep", tp),
            P(("y", "core", "ep")),
        ),
        check_vma=False,
    )
```

```python
import functools

import jax
import jax.numpy as jnp
from jax import lax
from jax.experimental import pallas as pl
from jax.experimental.pallas import tpu as pltpu
from jax.sharding import Mesh, PartitionSpec as P

BF = jnp.bfloat16
F32 = jnp.float32
LANES = 128


def up(n, k):
    return -(-n // k) * k


def nn(a, b):
    return lax.dot_general(a, b, (((1,), (0,)), ((), ())), preferred_element_type=F32)


def nt(a, b):
    return lax.dot_general(a, b, (((1,), (1,)), ((), ())), preferred_element_type=F32)


def tn(a, b):
    return lax.dot_general(a, b, (((0,), (0,)), ((), ())), preferred_element_type=F32)


def rows_of(shape):
    return lax.broadcasted_iota(jnp.int32, shape, 0)


def cols_of(shape):
    return lax.broadcasted_iota(jnp.int32, shape, 1)


def divided(n, by):
    return ((n.astype(F32) + 0.5) * (1.0 / by)).astype(jnp.int32)


def picked(mask):
    return mask.astype(F32).astype(BF)


def groups_of(experts):
    return 8 if experts % 8 == 0 else experts


def regroup(cap, group, to_kinds):
    size, count = 4 * cap * group, cap * group
    kinds, sources = rows_of((size, size)), cols_of((size, size))
    if not to_kinds:
        kinds, sources = sources, kinds
    kind = divided(kinds, count)
    kinds = kinds - kind * count
    source = divided(kinds, cap)
    return picked(sources == source * (3 * cap) + kinds + kind * cap)


def dispatch_kernel(experts, cap, share_ref, routes_ref, gates_ref, tok0, tok1, cot0, cot1, send_ref, rank_ref):
    toks = routes_ref.shape[1]
    slots = experts * cap
    route = [routes_ref[k : k + 1, :] for k in range(2)]
    ids = rows_of((experts, toks))
    named = [ids == r for r in route]
    both = picked(named[0] | named[1])
    before = picked(rows_of((toks, toks)) < cols_of((toks, toks)))
    earlier = nn(both, before)
    ranks = [jnp.sum(jnp.where(m, earlier, 0.0), axis=0, keepdims=True).astype(jnp.int32) for m in named]
    rank_ref[...] = jnp.concatenate(ranks, axis=0)
    slot = rows_of((slots, toks))
    same = rows_of((toks, toks)) == cols_of((toks, toks))
    toks_both = jnp.concatenate([tok0[...], tok1[...]], axis=1)
    cots_both = jnp.concatenate([cot0[...], cot1[...]], axis=1).astype(F32)
    rows_x = rows_c = None
    for k in range(2):
        at = picked(slot == route[k] * cap + ranks[k])
        gate = jnp.sum(jnp.where(same, gates_ref[k : k + 1, :], 0.0), axis=1, keepdims=True)
        x, c = nn(at, toks_both), nn(at, (gate * cots_both).astype(BF))
        rows_x, rows_c = (x, c) if rows_x is None else (rows_x + x, rows_c + c)
    rows_x, rows_c = rows_x.astype(BF), rows_c.astype(BF)
    group = groups_of(experts)
    order = regroup(cap, group, False)
    size, count = 4 * cap * group, cap * group
    for g in range(experts // group):
        rows = slice(g * count, (g + 1) * count)
        kinds = [m[rows, n * LANES : (n + 1) * LANES] for n in range(2) for m in (rows_x, rows_c)]
        send_ref[g * size : (g + 1) * size, :] = nn(order, jnp.concatenate(kinds, axis=0)).astype(BF)


def compact_kernel(cap, recv_ref, keep_ref, taken_ref, up_ref, down_ref, far_up_ref, far_down_ref, stay_ref):
    experts = recv_ref.shape[0] // (4 * cap)
    slots = experts * cap
    toks = keep_ref.shape[1]
    group = groups_of(experts)
    size, count = 4 * cap * group, cap * group
    order = regroup(cap, group, True)
    for g in range(experts // group):
        rows = nn(order, recv_ref[g * size : (g + 1) * size, :]).astype(BF)
        for n in range(4):
            at = slice(n * slots + g * count, n * slots + (g + 1) * count)
            part = rows[n * count : (n + 1) * count, :]
            up_ref[at, :] = part
            down_ref[at, :] = part
            if n < 2:
                far_up_ref[at, :] = part
                far_down_ref[at, :] = part
    near, far = 4 * slots, 2 * slots
    for n, (ref, at) in enumerate(
        ((up_ref, near), (up_ref, near + toks), (down_ref, near), (down_ref, near + toks), (far_up_ref, far), (far_down_ref, far))
    ):
        ref[at : at + toks, :] = (keep_ref[n].astype(F32) + taken_ref[n].astype(F32)).astype(BF)
    for n in range(2):
        stay_ref[n] = keep_ref[6 + n].astype(F32) + taken_ref[6 + n].astype(F32)


def join_kernel(mine_ref, up_ref, down_ref, far_up_ref, far_down_ref, stay_ref, own_ref, near_ref, far_ref):
    rows = own_ref.shape[1]
    toks = near_ref.shape[0]
    at = 0
    for ref, count in ((mine_ref, 2), (up_ref, 2), (down_ref, 2), (far_up_ref, 1), (far_down_ref, 1)):
        for n in range(count):
            own_ref[at] = ref[n * rows : (n + 1) * rows, :]
            at += 1
    near = stay_ref[0]
    for ref, count in ((up_ref, 2), (down_ref, 2), (far_up_ref, 1), (far_down_ref, 1)):
        near = near + ref[count * rows : count * rows + toks, :].astype(F32)
    near_ref[...] = near
    far = stay_ref[1]
    for ref in (up_ref, down_ref):
        far = far + ref[2 * rows + toks : 2 * rows + 2 * toks, :].astype(F32)
    far_ref[...] = far.astype(BF)


def swiglu_back(x, c, gate_weight, up_weight, down_weight):
    pre_gate = nt(gate_weight, x)
    pre_up = nt(up_weight, x)
    hidden_grad = nt(down_weight, c)
    s = jax.nn.sigmoid(pre_gate)
    activated = pre_gate * s
    hidden = (activated * pre_up).astype(BF)
    d_gate = (hidden_grad * pre_up * s * (1.0 + pre_gate * (1.0 - s))).astype(BF)
    d_up = (hidden_grad * activated).astype(BF)
    return hidden, hidden_grad, d_gate, d_up


ORDER = (1, 5, 7, 3, 2, 6, 0, 4)


def shared_kernel(
    at_ref, tok_ref, cot_ref, gate_ref, up_ref, down_ref, keep_ref, send_ref, term_ref, lined_ref, blocks_ref
):
    tok, cot = tok_ref[...], cot_ref[...]
    gate_weight, up_weight = gate_ref[...], up_ref[...]
    hidden, _, d_gate, d_up = swiglu_back(tok, cot, gate_weight, up_weight, down_ref[...])
    back = tn(
        jnp.concatenate([d_gate, d_up], axis=0), jnp.concatenate([gate_weight, up_weight], axis=0)
    ).astype(BF)
    term = nn(hidden, cot)
    for p in range(blocks_ref.shape[0]):
        blocks_ref[p] = back[:, p * LANES : (p + 1) * LANES]
        lined_ref[:, p, :] = term[:, p * LANES : (p + 1) * LANES]
    term_ref[...] = lined_ref[...].reshape(term_ref.shape).astype(BF)
    y, core = at_ref[0] >> 1, at_ref[0] & 1
    for n, offset in enumerate(ORDER):
        chip = lax.rem(y + offset, len(ORDER))
        keep_ref[n] = blocks_ref[2 * chip + core]
        send_ref[n] = blocks_ref[2 * chip + 1 - core]


OFFSETS = (0, 4, 7, 3, 1, 5, 6, 2)


def assemble(at_ref, own_ref, other_ref, x_ref, c_ref):
    slots = c_ref.shape[0]
    y, core = at_ref[0] >> 1, at_ref[0] & 1
    for n, offset in enumerate(OFFSETS):
        chip = lax.rem(y + offset, len(OFFSETS))
        for ref, side in ((own_ref, core), (other_ref, 1 - core)):
            lane = pl.multiple_of((2 * chip + side) * LANES, LANES)
            if x_ref is not None:
                x_ref[:, pl.ds(lane, LANES)] = ref[n, 0:slots, :]
            c_ref[:, pl.ds(lane, LANES)] = ref[n, slots : 2 * slots, :]


def lanes_of(refs, side, out_ref):
    at = 0
    for ref in refs:
        rows = ref.shape[0]
        for y in range(ref.shape[1] // (2 * LANES)):
            lane = pl.multiple_of((2 * y + side) * LANES, LANES)
            out_ref[at : at + rows, y * LANES : (y + 1) * LANES] = ref[:, pl.ds(lane, LANES)]
        at += rows


def expert_kernel(
    extra, at_ref, own_ref, other_ref, gate_ref, up_ref, down_ref,
    send_ref, dots_ref, hidden_ref, joined_ref, x_ref, c_ref, half_ref,
):
    assemble(at_ref, own_ref, other_ref, x_ref, c_ref)
    slots = x_ref.shape[0]
    hidden, hidden_grad, d_gate, d_up = swiglu_back(
        x_ref[...], c_ref[...], gate_ref[...], up_ref[...], down_ref[...]
    )
    hidden_ref[...] = hidden
    joined = jnp.concatenate([d_gate, d_up], axis=0)
    joined_ref[...] = joined
    lanes_of((gate_ref, up_ref), 1 - (at_ref[0] & 1), half_ref)
    back = tn(joined, half_ref[...]).astype(BF)
    dots = jnp.sum(hidden.astype(F32) * hidden_grad, axis=0, keepdims=True)
    wide = up(slots, LANES)
    dots = jnp.concatenate([dots, jnp.zeros((1, wide - slots), F32)], axis=1)
    line = rows_of((extra, LANES))
    rest = jnp.zeros((extra, LANES), F32)
    for k in range(wide // LANES):
        rest = jnp.where(line == k, dots[:, k * LANES : (k + 1) * LANES], rest)
    rest = rest.astype(BF)
    dots_ref[...] = rest
    for y in range(send_ref.shape[0]):
        send_ref[y, 0:slots, :] = back[:, y * LANES : (y + 1) * LANES]
        send_ref[y, slots : slots + extra, :] = rest


def keep_kernel(at_ref, x_ref, joined_ref, gate_ref, up_ref, keep_ref, g_gate_ref, g_up_ref, squares_ref, half_ref):
    units, width = g_gate_ref.shape
    shares = width // LANES
    joined = joined_ref[...]
    lanes_of((gate_ref, up_ref), at_ref[0] & 1, half_ref)
    back = tn(joined, half_ref[...]).astype(BF)
    for y in range(keep_ref.shape[0]):
        keep_ref[y] = back[:, y * LANES : (y + 1) * LANES]
    line = rows_of((2 * shares, LANES))
    rest = jnp.zeros((2 * shares, LANES), F32)
    for k, out_ref in enumerate((g_gate_ref, g_up_ref)):
        g = nn(joined[k * units : (k + 1) * units, :], x_ref[...])
        out_ref[...] = g
        sums = jnp.sum(g * g, axis=0, keepdims=True)
        for p in range(shares):
            rest = jnp.where(line == k * shares + p, sums[:, p * LANES : (p + 1) * LANES], rest)
    squares_ref[...] = rest.astype(BF)


def add_kernel(keep_ref, taken_ref, dots_ref, squares_ref, out_ref):
    slots = keep_ref.shape[1]
    rows = taken_ref.shape[1]
    dots, squares = dots_ref[...].astype(F32), squares_ref[...]
    for y in range(out_ref.shape[0]):
        out_ref[y, 0:slots, :] = (keep_ref[y].astype(F32) + taken_ref[y, 0:slots, :].astype(F32)).astype(BF)
        out_ref[y, slots:rows, :] = (dots + taken_ref[y, slots:rows, :].astype(F32)).astype(BF)
        out_ref[y, rows : rows + squares.shape[0], :] = squares


def down_kernel(at_ref, own_ref, other_ref, hidden_ref, g_down_ref, n_down_ref, c_ref):
    assemble(at_ref, own_ref, other_ref, None, c_ref)
    g_down = nn(hidden_ref[...], c_ref[...])
    g_down_ref[...] = g_down
    units = g_down.shape[0]
    n_down = jnp.sum(g_down * g_down, axis=1, keepdims=True) * (1.0 / g_down.shape[1])
    same = rows_of((units, units)) == cols_of((units, units))
    n_down_ref[...] = jnp.sum(jnp.where(same, n_down, 0.0), axis=0, keepdims=True)


def return_kernel(cap, block, parts_ref, back_ref, squares_ref):
    size = back_ref.shape[0]
    slots = size // block * cap
    total = parts_ref[0].astype(F32)
    for y in range(1, parts_ref.shape[0]):
        total = total + parts_ref[y].astype(F32)
    squares_ref[...] = total[total.shape[0] - squares_ref.shape[0] :, :]
    row = rows_of((size, slots))
    slot = cols_of((size, slots))
    source = divided(row, block)
    inner = row - source * block
    mask = (slot == source * cap + inner) & (inner < cap)
    back = nn(picked(mask), total[0:slots, :].astype(BF))
    row = rows_of((size, LANES))
    source = divided(row, block)
    is_dot = row == source * block + cap
    for k in range(up(slots, LANES) // LANES):
        dots = total[slots + k : slots + k + 1, :].astype(BF).astype(F32)
        mine = divided(cols_of((size, LANES)) + k * LANES, cap) == source
        left = jnp.where(is_dot & mine, dots, 0.0).astype(BF)
        number = rows_of((LANES, LANES)) + k * LANES
        place = number - divided(number, cap) * cap
        back = back + nn(left, picked(place == cols_of((LANES, LANES))))
    back_ref[...] = back.astype(BF)


def shared_sum_kernel(parts_ref, grad_ref, norm_ref):
    total = parts_ref[0].astype(F32)
    for e in range(1, parts_ref.shape[0]):
        total = total + parts_ref[e].astype(F32)
    rows, width = grad_ref.shape
    count = width // LANES
    lane = cols_of(norm_ref.shape)
    norm = jnp.zeros(norm_ref.shape, F32)
    for i in range(rows):
        mine = total[i * count : (i + 1) * count, :]
        for p in range(count):
            grad_ref[i : i + 1, p * LANES : (p + 1) * LANES] = mine[p : p + 1, :]
        square = jnp.sum(jnp.sum(mine * mine, axis=0, keepdims=True), axis=1, keepdims=True)
        norm = jnp.where(lane == i, square * (1.0 / width), norm)
    norm_ref[...] = norm


def combine_kernel(cap, block, recv_ref, routes_ref, rank_ref, gates_ref, near_ref, far_ref, grad_ref, gate_grad_ref):
    size = recv_ref.shape[0]
    toks = routes_ref.shape[1]
    recv = recv_ref[...]
    row = rows_of((size, toks))
    lane = rows_of((LANES, toks))
    at = []
    for k in range(2):
        route, rank = routes_ref[k : k + 1, :], rank_ref[k : k + 1, :]
        at.append(row == route * block + rank)
        dots = tn(recv, picked(row == route * block + cap))
        dot = jnp.sum(jnp.where(lane == rank, dots, 0.0), axis=0, keepdims=True)
        gate_grad_ref[k : k + 1, :] = dot / gates_ref[k : k + 1, :]
    grad_ref[...] = (tn(picked(at[0] | at[1]), recv) + (near_ref[...] + far_ref[...].astype(F32))).astype(BF)


def local(body, args, outs, scratch=(), scalars=0, flops=2 * 10**9):
    specs = [pl.BlockSpec(memory_space=pltpu.SMEM)] * scalars
    specs = specs + [pl.BlockSpec(memory_space=pltpu.VMEM)] * (len(args) - scalars)
    return pl.pallas_call(
        body,
        in_specs=specs,
        out_shape=tuple(jax.ShapeDtypeStruct(s, d) for s, d in outs),
        out_specs=tuple(pl.BlockSpec(memory_space=pltpu.VMEM) for _ in outs),
        scratch_shapes=list(scratch),
        cost_estimate=pl.CostEstimate(flops=flops, bytes_accessed=flops // 500, transcendentals=0),
        compiler_params=pltpu.CompilerParams(vmem_limit_bytes=20 * 1024 * 1024),
    )(*args)


def shifted(x, by, count):
    return lax.ppermute(x, "y", [(i, (i + by) % count) for i in range(count)])


def all_steps(tokens, routes, route_gates, cotangent, w_gate, w_up, w_down, s_gate, s_up, s_down):
    tp = ("y", "core")
    ep_count = lax.axis_size("ep")
    shares = lax.axis_size(tp)
    chips = shares // 2
    at = lax.axis_index(tp).astype(jnp.int32).reshape(1)
    toks, width = tokens.shape
    units = w_gate.shape[2]
    cap = max(2, (9 * toks * 2 + 8 * ep_count - 1) // (8 * ep_count))
    slots = ep_count * cap
    back_block = up(cap + 1, 8)
    routes_t, gates_t = routes.T, route_gates.T

    narrow = [pl.BlockSpec((toks, LANES), lambda i, s, n=n: (0, lax.rem(s[0] + n * chips, shares))) for n in range(2)]
    whole = pl.BlockSpec((2, toks), lambda i, s: (0, 0))
    send, ranks = pl.pallas_call(
        functools.partial(dispatch_kernel, ep_count, cap),
        out_shape=(
            jax.ShapeDtypeStruct((4 * slots, LANES), BF),
            jax.ShapeDtypeStruct((2, toks), jnp.int32),
        ),
        grid_spec=pltpu.PrefetchScalarGridSpec(
            num_scalar_prefetch=1,
            grid=(1,),
            in_specs=[whole, whole] + narrow + narrow,
            out_specs=(
                pl.BlockSpec((4 * slots, LANES), lambda i, s: (0, 0)),
                pl.BlockSpec((2, toks), lambda i, s: (0, 0)),
            ),
        ),
    )(at, routes_t, gates_t, tokens, tokens, cotangent, cotangent)
    recv = lax.all_to_all(send.reshape(ep_count, 4 * cap, LANES), "ep", 0, 0, tiled=True)

    keep, give, term = local(
        shared_kernel,
        (at, tokens, cotangent, s_gate.T, s_up.T, s_down),
        [((chips, toks, LANES), BF)] * 2 + [((ep_count, units * shares // ep_count, LANES), BF)],
        [pltpu.VMEM((units, shares, LANES), F32), pltpu.VMEM((shares, toks, LANES), BF)],
        scalars=1,
        flops=4 * 10**9,
    )
    swap = [(0, 1), (1, 0)]
    taken = lax.ppermute(give, "core", swap)
    recv, keep, taken, term = lax.optimization_barrier((recv, keep, taken, term))
    term_parts = lax.all_to_all(term, "ep", 0, 0, tiled=True)

    near, far = 4 * slots, 2 * slots
    go_up, go_down, go_far_up, go_far_down, stay = local(
        functools.partial(compact_kernel, cap),
        (recv.reshape(4 * slots, LANES), keep, taken),
        [((near + 2 * toks, LANES), BF)] * 2 + [((far + toks, LANES), BF)] * 2 + [((2, toks, LANES), F32)],
    )
    came_up = shifted(go_up, 1, chips)
    came_down = shifted(go_down, -1, chips)
    came_far_up = shifted(go_far_up, 2, chips)
    came_far_down = shifted(go_far_down, -2, chips)
    own, shared_near, shared_far = local(
        join_kernel,
        (go_up, came_up, came_down, came_far_up, came_far_down, stay),
        [((chips, far, LANES), BF), ((toks, LANES), F32), ((toks, LANES), BF)],
    )
    other = lax.ppermute(own, "core", swap)
    shared_far = shifted(shared_far, chips // 2, chips)

    extra = up(up(slots, LANES) // LANES, 8)
    weights = (w_gate[0].T, w_up[0].T)
    half = pltpu.VMEM((2 * units, width // 2), BF)
    give, dots, hidden, joined, x = local(
        functools.partial(expert_kernel, extra),
        (at, own, other, *weights, w_down[0]),
        [
            ((chips, slots + extra, LANES), BF),
            ((extra, LANES), BF),
            ((units, slots), BF),
            ((2 * units, slots), BF),
            ((slots, width), BF),
        ],
        [pltpu.VMEM((slots, width), BF), half],
        scalars=1,
        flops=6 * 10**9,
    )
    taken = lax.ppermute(give, "core", swap)
    grads = ((units, width), F32)
    keep, g_gate, g_up, squares = local(
        keep_kernel,
        (at, x, joined, *weights),
        [((chips, slots, LANES), BF), grads, grads, ((2 * shares, LANES), BF)],
        [half],
        scalars=1,
        flops=4 * 10**9,
    )
    (pair,) = local(
        add_kernel, (keep, taken, dots, squares), [((chips, slots + extra + 2 * shares, LANES), BF)]
    )
    pair_parts = lax.all_to_all(pair, "y", 0, 0, tiled=True)

    g_down, n_down = local(
        down_kernel,
        (at, own, other, hidden),
        [grads, ((1, units), F32)],
        [pltpu.VMEM((slots, width), BF)],
        scalars=1,
        flops=3 * 10**9,
    )
    back, squares = local(
        functools.partial(return_kernel, cap, back_block),
        (pair_parts,),
        [((ep_count * back_block, LANES), BF), ((2 * shares, LANES), F32)],
    )
    squares = squares + lax.ppermute(squares, "core", swap)
    norm_in = (squares * (1.0 / (units * shares))).reshape(2, width)
    came = lax.all_to_all(back.reshape(ep_count, back_block, LANES), "ep", 0, 0, tiled=True)
    token_grad, gate_grad = local(
        functools.partial(combine_kernel, cap, back_block),
        (came.reshape(ep_count * back_block, LANES), routes_t, ranks, gates_t, shared_near, shared_far),
        [((toks, LANES), BF), ((2, toks), F32)],
    )

    grad_shared, norm_shared = local(
        shared_sum_kernel, (term_parts,), [((term.shape[1] * LANES // width, width), F32), ((1, term.shape[1] * LANES // width), F32)]
    )
    norm_shared = norm_shared.reshape(-1)
    return (
        token_grad,
        gate_grad.T,
        g_gate.T[None],
        g_up.T[None],
        g_down[None],
        grad_shared,
        norm_in[None],
        n_down,
        norm_shared,
    )


def solution(mesh):
    tp = ("y", "core")
    ep_count, tp_count = mesh.devices.shape
    fine = Mesh(mesh.devices.reshape(ep_count, tp_count // 2, 2), ("ep", "y", "core"))
    placed = (
        P("ep", None),
        P("ep", None),
        P("ep", None),
        P("ep", None),
        P("ep", None, tp),
        P("ep", None, tp),
        P("ep", tp, None),
        P(None, tp),
        P(None, tp),
        P(tp, None),
    )
    return jax.shard_map(
        all_steps,
        mesh=fine,
        in_specs=placed,
        out_specs=(
            P("ep", tp),
            P("ep", None),
            P("ep", None, tp),
            P("ep", None, tp),
            P("ep", tp, None),
            P(("y", "core", "ep"), None),
            P("ep", None, None),
            P("ep", tp),
            P(("y", "core", "ep")),
        ),
        check_vma=False,
    )
```
